512 devices in a mesh: sp: 16 (over z), dp: 32 (over y, x, core).
Axes of the slice: x: 4, y: 4, z: 16, core: 2. Of those that a mesh axis runs over, the one named last changes fastest.
Arguments:
- query_latent: bfloat16 [32, 2048, 768], P('dp', 'sp'), may hold values from -6 to 6
- keyvalue_latent: bfloat16 [32, 2048, 512], P('dp', 'sp'), may hold values from -6 to 6
- rope_key: bfloat16 [32, 2048, 32], P('dp', 'sp'), may hold values from -150 to 150
- query_gain: float32 [768], replicated, may hold values from 0.1 to 1.9
- keyvalue_gain: float32 [512], replicated, may hold values from 0.1 to 1.9
- narrow_query: bfloat16 [768, 1536], P('dp'), may hold values from -0.21875 to 0.21875
- broad_query: bfloat16 [768, 2560], P('dp'), may hold values from -0.21875 to 0.21875
- narrow_key: bfloat16 [512, 1024], P('dp'), may hold values from -0.25 to 0.25
- narrow_value: bfloat16 [512, 1024], P('dp'), may hold values from -0.25 to 0.25
- broad_key: bfloat16 [512, 2048], P('dp'), may hold values from -0.25 to 0.25
- broad_value: bfloat16 [512, 1024], P('dp'), may hold values from -0.25 to 0.25
Outputs:
- narrow_mixed: bfloat16 [32, 2048, 1024], P('dp', 'sp')
- broad_mixed: bfloat16 [32, 2048, 1024], P('dp', 'sp')
The draws below stay inside these ranges and needn't reach their ends.
All inputs are finite; a program needn't handle non-finite values.
Results may differ from the reference program's by a relative error of at most 0.014.
The reference program's roundings to bfloat16 on the way count: a program that leaves them out, or rounds other values in their place, can miss the bound.
Values may be sent and summed in bfloat16 or wider, within the bound.
A program may use at most 64 MiB of HBM per device.

```python
import jax
import jax.numpy as jnp
from jax import lax

QUERY_RANK = 768
PAIR_RANK = 512
PLAIN_NARROW = 64
PLAIN_BROAD = 128
ROTARY = 32
VALUE_SIZE = 64
HEADS = 16
LENGTH = 2048
SEQS = 32


def draw_rope_key(key, part):
    base_key = jax.random.fold_in(key, 11)
    values = jnp.clip(jax.random.normal(base_key, (SEQS, LENGTH, ROTARY), jnp.float32), -6.0, 6.0)
    return values.astype(jnp.bfloat16)


def level_of(key, shape, split, smallest, high):
    loudness = 1.0
    for position, shards_of in split:
        draws = jax.random.uniform(jax.random.fold_in(jax.random.fold_in(key, 6), position), (shards_of,), jnp.float32, smallest / len(split), high / len(split))
        loudness = loudness * jnp.repeat(jnp.exp(draws), shape[position] // shards_of).reshape((-1,) + (1,) * (len(shape) - 1 - position))
    return loudness


def normal_values(rng, extent, spread, limit, shards=(), held_as=jnp.bfloat16):
    array = spread * jax.random.normal(rng, extent, jnp.float32)
    if shards:
        array = array * level_of(rng, extent, shards, -0.22, 0.18)
    return jnp.clip(array, -limit, limit).astype(held_as)


def setup_inputs(seed: int = 0) -> dict:
    arg_keys = jax.random.split(jax.random.key(seed), 12)
    return {
        "query_latent": normal_values(arg_keys[0], (SEQS, LENGTH, QUERY_RANK), 1.0, 6.0, ((0, 32), (1, 16))),
        "keyvalue_latent": normal_values(arg_keys[1], (SEQS, LENGTH, PAIR_RANK), 1.0, 6.0, ((0, 32), (1, 16))),
        "rope_key": draw_rope_key(jax.random.fold_in(arg_keys[11], 71), 0),
        "query_gain": jnp.clip(1.0 + 0.18 * jax.random.normal(arg_keys[3], (QUERY_RANK,), jnp.float32), 0.1, 1.9),
        "keyvalue_gain": jnp.clip(1.0 + 0.18 * jax.random.normal(arg_keys[4], (PAIR_RANK,), jnp.float32), 0.1, 1.9),
        "narrow_query": normal_values(arg_keys[5], (QUERY_RANK, HEADS * (PLAIN_NARROW + ROTARY)), QUERY_RANK ** -0.5, 0.21875, ((0, 32),)),
        "broad_query": normal_values(arg_keys[6], (QUERY_RANK, HEADS * (PLAIN_BROAD + ROTARY)), QUERY_RANK ** -0.5, 0.21875, ((0, 32),)),
        "narrow_key": normal_values(arg_keys[7], (PAIR_RANK, HEADS * PLAIN_NARROW), PAIR_RANK ** -0.5, 0.25, ((0, 32),)),
        "narrow_value": normal_values(arg_keys[8], (PAIR_RANK, HEADS * VALUE_SIZE), PAIR_RANK ** -0.5, 0.25, ((0, 32),)),
        "broad_key": normal_values(arg_keys[9], (PAIR_RANK, HEADS * PLAIN_BROAD), PAIR_RANK ** -0.5, 0.25, ((0, 32),)),
        "broad_value": normal_values(arg_keys[10], (PAIR_RANK, HEADS * VALUE_SIZE), PAIR_RANK ** -0.5, 0.25, ((0, 32),)),
    }


EPSILON = 1e-06
ROTARY_BASE = 10000.0

def normalize(latent, gain_row):
    values = latent.astype(jnp.float32)
    scaled = values * lax.rsqrt(lax.optimization_barrier(jnp.mean(values * values, axis=-1, keepdims=True)) + EPSILON)
    return (scaled * gain_row.astype(jnp.float32)).astype(jnp.bfloat16)

def rotate(values, positions):
    halfway = ROTARY // 2
    frequency = ROTARY_BASE ** (-jnp.arange(halfway, dtype=jnp.float32) / halfway)
    angles = positions[:, None] * frequency[None, :]
    cosine = jnp.cos(angles)[:, None, :]
    sine_part = jnp.sin(angles)[:, None, :]
    width = values.shape[-1]
    plain_part = values[..., :width - ROTARY]
    first_half = values[..., width - ROTARY:width - halfway]
    second_half = values[..., width - halfway:]
    return jnp.concatenate([plain_part, first_half * cosine - second_half * sine_part, first_half * sine_part + second_half * cosine], axis=-1)

def attend_group(queries, keys_plain, values, rope_keys, factor):

    def one_head(members):
        query_head, key_head, value_head = members
        key_whole = jnp.concatenate([key_head, rope_keys], axis=1)
        scores = jnp.dot(query_head, key_whole.T, preferred_element_type=jnp.float32) * factor
        shifted = jnp.exp(scores - lax.optimization_barrier(jnp.max(scores, axis=-1, keepdims=True)))
        totals = lax.optimization_barrier(jnp.sum(shifted, axis=-1, keepdims=True))
        mixed = jnp.dot(shifted.astype(jnp.bfloat16), value_head, preferred_element_type=jnp.float32)
        return (mixed / totals).astype(jnp.bfloat16)
    stacked = lax.map(one_head, (jnp.swapaxes(queries, 0, 1), jnp.swapaxes(keys_plain, 0, 1), jnp.swapaxes(values, 0, 1)))
    return jnp.swapaxes(stacked, 0, 1)

def group_norm(attended):
    flattened = attended.reshape(attended.shape[0], -1).astype(jnp.float32)
    scaled = flattened * lax.rsqrt(lax.optimization_barrier(jnp.mean(flattened * flattened, axis=-1, keepdims=True)) + EPSILON)
    return scaled.astype(jnp.bfloat16)

def reference(query_latent, keyvalue_latent, rope_key, query_gain, keyvalue_gain, narrow_query, broad_query, narrow_key, narrow_value, broad_key, broad_value):

    def one_sequence(members):
        query_rows, pair_rows, rope_rows = members
        length = query_rows.shape[0]
        positions = jnp.arange(length).astype(jnp.float32)
        query_normed = normalize(query_rows, query_gain)
        pair_normed = normalize(pair_rows, keyvalue_gain)
        rope_keys = rotate(rope_rows.astype(jnp.float32)[:, None, :], positions)[:, 0, :].astype(jnp.bfloat16)
        width_narrow = PLAIN_NARROW + ROTARY
        width_broad = PLAIN_BROAD + ROTARY
        query_first = rotate(jnp.dot(query_normed, narrow_query, preferred_element_type=jnp.float32).reshape(length, HEADS, width_narrow), positions).astype(jnp.bfloat16)
        query_second = rotate(jnp.dot(query_normed, broad_query, preferred_element_type=jnp.float32).reshape(length, HEADS, width_broad), positions).astype(jnp.bfloat16)
        key_first = jnp.dot(pair_normed, narrow_key, preferred_element_type=jnp.float32).astype(jnp.bfloat16).reshape(length, HEADS, PLAIN_NARROW)
        value_first = jnp.dot(pair_normed, narrow_value, preferred_element_type=jnp.float32).astype(jnp.bfloat16).reshape(length, HEADS, VALUE_SIZE)
        key_second = jnp.dot(pair_normed, broad_key, preferred_element_type=jnp.float32).astype(jnp.bfloat16).reshape(length, HEADS, PLAIN_BROAD)
        value_second = jnp.dot(pair_normed, broad_value, preferred_element_type=jnp.float32).astype(jnp.bfloat16).reshape(length, HEADS, VALUE_SIZE)
        mixed_first = attend_group(query_first, key_first, value_first, rope_keys, width_narrow ** (-0.5))
        mixed_second = attend_group(query_second, key_second, value_second, rope_keys, width_broad ** (-0.5))
        return (group_norm(mixed_first), group_norm(mixed_second))
    narrow_mixed, broad_mixed = lax.map(one_sequence, (query_latent, keyvalue_latent, rope_key))
    return (narrow_mixed, broad_mixed)
```

```python
import functools
import math

import jax
import jax.numpy as jnp
import numpy as np
from jax import lax
from jax.experimental import pallas as pl
from jax.experimental.pallas import tpu as pltpu
from jax.sharding import PartitionSpec as P

EPSILON = 1e-06
ROTARY_BASE = 10000.0
NZ = 16
NXY = 16
PXY = 4
PZ = 4
BF = jnp.bfloat16
F32 = jnp.float32
MESH = pl.DeviceIdType.MESH
NARROW_SCALE = 96 ** -0.5 * math.log2(math.e)
BROAD_SCALE = 160 ** -0.5 * math.log2(math.e)
KEY_BLOCK = 512


def rotary_tables():
    frequency = ROTARY_BASE ** (-np.arange(16, dtype=np.float64) / 16)
    lanes = np.tile(frequency, 8)
    coarse = (256.0 * np.arange(8))[:, None] * lanes[None, :]
    fine = np.arange(256.0)[:, None] * lanes[None, :]
    return tuple(
        np.asarray(t, np.float32)
        for t in (np.cos(coarse), np.sin(coarse), np.cos(fine), np.sin(fine))
    )


def lane_iota(shape):
    return lax.broadcasted_iota(jnp.int32, shape, len(shape) - 1)


def row_iota(shape):
    return lax.broadcasted_iota(jnp.int32, shape, 0)


def normalize(latent, gain_row):
    values = latent.astype(F32)
    scaled = values * lax.rsqrt(jnp.mean(values * values, axis=-1, keepdims=True) + EPSILON)
    return (scaled * gain_row).astype(BF)


def rotate(values, cosine, signed_sine):
    first = lane_iota(values.shape) % 32 < 16
    swapped = jnp.where(first, pltpu.roll(values, 112, 1), pltpu.roll(values, 16, 1))
    return values * cosine + swapped * signed_sine


def take(columns, segments):
    rows = columns.shape[0]
    lane = lane_iota((rows, 128))
    out, dest = None, 0
    for start, width in segments:
        tile, off = start // 128, start % 128
        span = 128 if off + width <= 128 else 256
        window = columns[:, tile * 128 : tile * 128 + span]
        shift = (dest - off) % span
        moved = pltpu.roll(window, shift, 1)[:, :128] if shift else window[:, :128]
        out = moved if out is None else jnp.where(lane >= dest, moved, out)
        dest += width
    return out


def ring_chip(ring, position):
    major = position // 4
    minor = lax.rem(position - major + 16, 4)
    return (minor, major) if ring == 0 else (major, minor)


def body(
    ql, kl, rk, qg, kg, ca, sa, cb, sb, nq, bq, nk, nv, bk, bv,
    out_n, out_b,
    raw_n, raw_b, wq8, wkv, kv, rt, qn, wq, wvt, qmt, kp, kr, vt, at, sbuf, cos_t, sin_t,
    in_sem, xy_send, xy_recv, dd_send, dd_recv, z_send, z_recv, zr_send, zr_recv,
    q_send, q_recv, o_send, o_recv,
):
    z = lax.axis_index("sp")
    d = lax.axis_index("dp")
    par = lax.rem(z, 2)
    core = lax.rem(d, 2)
    chip = d // 2
    cx, cy = lax.rem(chip, 4), chip // 4
    diag = lax.rem(cx + cy, 4)
    ring_pos = (4 * cy + diag, 4 * cx + diag)
    partner_core = d + 1 - 2 * core
    mate = z + 1 - 2 * par

    def slot_of(ring, position):
        x, y = ring_chip(ring, lax.rem(position + 32, 16))
        return (y * 4 + x) * 2 + core

    def cols(ref, width):
        return ref.at[:, pl.ds(pl.multiple_of(par * width, 128), width)]

    own_rows = pl.ds(pl.multiple_of(d * 16, 16), 16)
    loads = [
        pltpu.make_async_copy(cols(nq, 768), raw_n, in_sem.at[0]),
        pltpu.make_async_copy(cols(bq, 1280), raw_b, in_sem.at[1]),
        pltpu.make_async_copy(cols(nk, 512), wkv.at[own_rows, pl.ds(0, 512)], in_sem.at[2]),
        pltpu.make_async_copy(cols(bk, 1024), wkv.at[own_rows, pl.ds(512, 1024)], in_sem.at[3]),
        pltpu.make_async_copy(cols(nv, 512), wkv.at[own_rows, pl.ds(1536, 512)], in_sem.at[4]),
        pltpu.make_async_copy(cols(bv, 512), wkv.at[own_rows, pl.ds(2048, 512)], in_sem.at[5]),
    ]
    for load in loads:
        load.start()

    barrier = pltpu.get_barrier_semaphore()
    near = [{"sp": lax.rem(z + 1, 16)}, {"sp": lax.rem(z + 15, 16)}, {"dp": partner_core}]
    for ring in range(2):
        for step in (1, -1):
            near.append({"dp": slot_of(ring, ring_pos[ring] + step)})
    for who in near:
        pl.semaphore_signal(barrier, inc=1, device_id=who, device_id_type=MESH)

    kv[z] = normalize(kl[0], kg[...])
    half = pl.ds(pl.multiple_of(par * 128, 128), 128)
    coarse = pl.ds(z // 2, 1)
    cosine = ca[coarse, :] * cb[...] - sa[coarse, :] * sb[...]
    sine = sa[coarse, :] * cb[...] + ca[coarse, :] * sb[...]
    cos_t[...] = cosine
    sin_t[...] = jnp.where(lane_iota(sine.shape) % 32 < 16, -sine, sine)
    spread = (row_iota((32, 128)) == lane_iota((32, 128)) % 32).astype(BF)
    rope4 = jnp.dot(rk[0], spread, preferred_element_type=F32)
    rope4 = rotate(rope4, cos_t[half, :], sin_t[half, :])
    rt[z] = rope4.T[:32].astype(BF)
    qn[par] = normalize(ql[0], qg[...])
    for load in loads:
        load.wait()
    wn, wb = raw_n[...].astype(F32), raw_b[...].astype(F32)
    blocks = [take(wn, [(192 * j, 64), (192 * j + 96, 64)]) for j in range(4)]
    blocks += [take(wb, [(160 * h, 128)]) for h in range(8)]
    blocks += [take(wn, [(96 * h + 64, 32) for h in range(4 * g, 4 * g + 4)]) for g in range(2)]
    blocks += [take(wb, [(160 * h + 128, 32) for h in range(4 * g, 4 * g + 4)]) for g in range(2)]
    for i, block in enumerate(blocks):
        for t in range(3):
            wq8[3 * d + t, :, 128 * i : 128 * i + 128] = block[8 * t : 8 * t + 8].astype(BF)

    pl.semaphore_wait(barrier, 7)

    def unit(ring, slot):
        if ring == 0:
            return wq8.at[pl.ds(3 * slot, 3)]
        return wkv.at[pl.ds(pl.multiple_of(16 * slot, 16), 16)]

    def piece(ring, slot, i):
        if ring == 0:
            return wq8.at[pl.ds(3 * slot, 3), :, pl.ds(i * (2048 // PXY), 2048 // PXY)]
        rows = pl.ds(pl.multiple_of(16 * slot, 16), 16)
        return wkv.at[rows, pl.ds(i * (2560 // PXY), 2560 // PXY)]

    def xy_copy(ring, way, step, i):
        sign = 1 - 2 * way
        slot = slot_of(ring, ring_pos[ring] - sign * (step - 1))
        ref = piece(ring, slot, i)
        flow = 2 * ring + way
        index = (step - 1) * PXY + i
        to = slot_of(ring, ring_pos[ring] + sign)
        return pltpu.make_async_remote_copy(
            ref, ref, xy_send.at[flow, index], xy_recv.at[flow, index],
            device_id={"dp": to}, device_id_type=MESH,
        )

    def xy_landed(ring, way, step, i):
        sign = 1 - 2 * way
        slot = slot_of(ring, ring_pos[ring] - sign * step)
        ref = piece(ring, slot, i)
        flow = 2 * ring + way
        index = (step - 1) * PXY + i
        pltpu.make_async_remote_copy(
            ref, ref, xy_send.at[flow, index], xy_recv.at[flow, index],
            device_id={"dp": d}, device_id_type=MESH,
        ).wait_recv()

    def dd_copy(ring, offset):
        slot = slot_of(ring, ring_pos[ring] + offset)
        ref = unit(ring, slot)
        index = offset + 7
        return pltpu.make_async_remote_copy(
            ref, ref, dd_send.at[ring, index], dd_recv.at[ring, index],
            device_id={"dp": partner_core}, device_id_type=MESH,
        )

    def dd_landed(ring, offset):
        x, y = ring_chip(ring, lax.rem(ring_pos[ring] + offset + 32, 16))
        ref = unit(ring, (y * 4 + x) * 2 + 1 - core)
        index = offset + 7
        pltpu.make_async_remote_copy(
            ref, ref, dd_send.at[ring, index], dd_recv.at[ring, index],
            device_id={"dp": partner_core}, device_id_type=MESH,
        ).wait_recv()

    rows_z = 128 // PZ

    def z_ref(slot, i):
        return rt.at[slot] if i == PZ else kv.at[slot, pl.ds(i * rows_z, rows_z)]

    def z_desc(way, step, i, slot):
        ref = z_ref(slot, i)
        sign = 1 - 2 * way
        index = (step - 1) * (PZ + 1) + i
        return pltpu.make_async_remote_copy(
            ref, ref, z_send.at[way, index], z_recv.at[way, index],
            device_id={"sp": lax.rem(z + sign + 16, 16)}, device_id_type=MESH,
        )

    def z_copy(way, step, i):
        return z_desc(way, step, i, lax.rem(z - (1 - 2 * way) * (step - 1) + 32, 16))

    def z_landed(way, step, i):
        z_desc(way, step, i, lax.rem(z - (1 - 2 * way) * step + 32, 16)).wait_recv()

    def xy_pieces(way, step):
        if step < 8:
            return list(range(PXY))
        return list(range(PXY // 2)) if way == 0 else list(range(PXY // 2, PXY))

    def z_pieces(way, step):
        if step < 8:
            return [PZ] + list(range(PZ))
        return [PZ] + list(range(PZ // 2)) if way == 0 else list(range(PZ // 2, PZ))

    started = []

    def start(copy):
        copy.start()
        started.append(copy)

    for i in range(PXY):
        for ring in range(2):
            for way in range(2):
                start(xy_copy(ring, way, 1, i))
    for i in z_pieces(0, 1):
        for way in range(2):
            start(z_copy(way, 1, i))
    for ring in range(2):
        start(dd_copy(ring, 0))
    mine = qn.at[par]
    q_copy = pltpu.make_async_remote_copy(
        mine, mine, q_send.at[0], q_recv.at[0], device_id={"sp": mate}, device_id_type=MESH
    )
    start(q_copy)

    def xy_event(step, i):
        for ring in range(2):
            for way in range(2):
                if i not in xy_pieces(way, step):
                    continue
                xy_landed(ring, way, step, i)
                if step < 8 and i in xy_pieces(way, step + 1):
                    start(xy_copy(ring, way, step + 1, i))
                if step < 8 and i == PXY - 1:
                    start(dd_copy(ring, (2 * way - 1) * step))
            if step == 8 and i == PXY - 1:
                start(dd_copy(ring, 8))

    def z_event(step, i):
        for way in range(2):
            if i not in z_pieces(way, step):
                continue
            z_landed(way, step, i)
            if step < 8 and i in z_pieces(way, step + 1):
                start(z_copy(way, step + 1, i))

    events = []
    for step in range(1, 9):
        for i in range(PXY):
            events.append((2.1 * (step - 1) + 2.1 * (i + 1) / PXY, xy_event, step, i))
        events.append((3.0 * (step - 1) + 0.2, z_event, step, PZ))
        for i in range(PZ):
            events.append((3.0 * (step - 1) + 3.0 * (i + 1) / PZ, z_event, step, i))
    for _, event, step, i in sorted(events, key=lambda e: e[0]):
        event(step, i)
    for ring in range(2):
        for offset in range(-7, 9):
            dd_landed(ring, offset)
    theirs = qn.at[1 - par]
    pltpu.make_async_remote_copy(
        theirs, theirs, q_send.at[0], q_recv.at[0], device_id={"sp": mate}, device_id_type=MESH
    ).wait_recv()

    def pack_rows(g, carry):
        pair = jnp.concatenate([wq8[2 * g].astype(F32), wq8[2 * g + 1].astype(F32)], axis=0)
        wq[pl.ds(pl.multiple_of(16 * g, 16), 16), :] = pair.astype(BF)
        return carry

    lax.fori_loop(0, 48, pack_rows, 0)
    for i in range(8):
        wvt[128 * i : 128 * i + 128, :] = wkv[:, 1536 + 128 * i : 1664 + 128 * i].T

    tokens = jnp.concatenate([qn[0], qn[1]], axis=0)
    group = row_iota((128, 256)) // 32
    side = row_iota((128, 256)) // 64
    nothing = jnp.zeros((128, 256), BF)
    for pair in range(8):
        both = jnp.dot(tokens, wq[:, 256 * pair : 256 * pair + 256], preferred_element_type=F32)
        for k in range(2):
            block = 2 * pair + k
            part = both[:, 128 * k : 128 * k + 128]
            if block >= 12:
                part = rotate(part, cos_t[...], sin_t[...])
            turned = part.astype(BF).T
            if block < 4:
                for s in range(2):
                    qmt[2 * block + s, 0:128, :] = jnp.where(side == s, turned, nothing)
            elif block < 12:
                qmt[block + 4, 0:128, :] = turned
            else:
                for g in range(4):
                    head = 4 * (block - 12) + g
                    qmt[head, 128:256, :] = jnp.where(group == g, turned, nothing)

    for h in range(16):
        vt[h, 64:80, :] = jnp.ones((16, 2048), BF)

    def project(b, carry):
        rows = pl.ds(pl.multiple_of(256 * b, 256), 256)
        x = jnp.concatenate([kv[2 * b], kv[2 * b + 1]], axis=0)
        for i in range(6):
            kp[rows, 256 * i : 256 * i + 256] = jnp.dot(
                x, wkv[:, 256 * i : 256 * i + 256], preferred_element_type=F32
            ).astype(BF)
        for i in range(4):
            turned = lax.dot_general(
                wvt[256 * i : 256 * i + 256, :], x, (((1,), (1,)), ((), ())),
                preferred_element_type=F32,
            ).astype(BF)
            for k in range(4):
                vt[4 * i + k, 0:64, rows] = turned[64 * k : 64 * k + 64]
        for k in range(2):
            one = rt[2 * b + k].astype(F32)
            kr[pl.ds(pl.multiple_of(256 * b + 128 * k, 128), 128), :] = (
                jnp.concatenate([one, one, one, one], axis=0).T.astype(BF)
            )
        return carry

    lax.fori_loop(0, 8, project, 0)

    def attend(h, factor, column):
        top = jnp.full((1, 256), -1e30, F32)
        total = jnp.zeros((80, 256), F32)
        operand = qmt[h]
        for b in range(2048 // KEY_BLOCK):
            rows = slice(b * KEY_BLOCK, (b + 1) * KEY_BLOCK)
            keys = jnp.concatenate([kp[rows, pl.ds(column, 128)], kr[rows, :]], axis=1)
            scores = jnp.dot(keys, operand, preferred_element_type=F32)
            new_top = jnp.maximum(top, jnp.max(scores, axis=0, keepdims=True))
            weights = jnp.exp2((scores - new_top) * factor).astype(BF)
            total = total * jnp.exp2((top - new_top) * factor) + jnp.dot(
                vt[h, :, rows], weights, preferred_element_type=F32
            )
            top = new_top
        return total[0:64] / total[64:65]

    def out_desc(j):
        broad = j // 4
        dst = 8 * broad + 4 * par + j - 4 * broad
        return pltpu.make_async_remote_copy(
            sbuf.at[j], at.at[dst], o_send.at[j], o_recv.at[j],
            device_id={"sp": mate}, device_id_type=MESH,
        )

    def two_heads(j, carry):
        broad = j // 4
        factor = jnp.where(broad == 0, NARROW_SCALE, BROAD_SCALE).astype(F32)
        parts = []
        for k in range(2):
            h = 2 * j + k
            block = (1 - broad) * j + broad * (h - 4)
            parts.append(attend(h, factor, pl.multiple_of(block * 128, 128)))
        stacked = jnp.concatenate(parts, axis=0).astype(BF)
        low, high = stacked[:, 0:128].T, stacked[:, 128:256].T
        even = par == 0
        at[8 * broad + 4 * par + j - 4 * broad] = jnp.where(even, low, high)
        sbuf[j] = jnp.where(even, high, low)
        out_desc(j).start()
        return carry

    lax.fori_loop(0, 8, two_heads, 0)

    def landed(j, carry):
        broad = j // 4
        src = 8 * broad + 4 * (1 - par) + j - 4 * broad
        pltpu.make_async_remote_copy(
            at.at[src], at.at[src], o_send.at[j], o_recv.at[j],
            device_id={"sp": mate}, device_id_type=MESH,
        ).wait_recv()
        out_desc(j).wait_send()
        return carry

    lax.fori_loop(0, 8, landed, 0)
    for which, out in enumerate((out_n, out_b)):
        values = [at[8 * which + i].astype(F32) for i in range(8)]
        squares = sum(v * v for v in values)
        mean = jnp.sum(squares, axis=-1, keepdims=True) * (1.0 / 1024)
        scale = lax.rsqrt(mean + EPSILON)
        for i in range(8):
            out[0, :, 128 * i : 128 * i + 128] = (values[i] * scale).astype(BF)

    for copy in started:
        copy.wait_send()


def on_device(ql, kl, rk, qg, kg, nq, bq, nk, nv, bk, bv):
    vmem = pl.BlockSpec(memory_space=pltpu.VMEM)
    hbm = pl.BlockSpec(memory_space=pl.ANY)
    dma = pltpu.SemaphoreType.DMA
    return pl.pallas_call(
        body,
        out_shape=[jax.ShapeDtypeStruct((1, 128, 1024), BF)] * 2,
        in_specs=[vmem] * 9 + [hbm] * 6,
        out_specs=[vmem] * 2,
        scratch_shapes=[
            pltpu.VMEM((24, 768), BF),
            pltpu.VMEM((24, 1280), BF),
            pltpu.VMEM((96, 8, 2048), BF),
            pltpu.VMEM((512, 2560), BF),
            pltpu.VMEM((16, 128, 512), BF),
            pltpu.VMEM((16, 32, 128), BF),
            pltpu.VMEM((2, 128, 768), BF),
            pltpu.VMEM((768, 2048), BF),
            pltpu.VMEM((1024, 512), BF),
            pltpu.VMEM((16, 256, 256), BF),
            pltpu.VMEM((2048, 1536), BF),
            pltpu.VMEM((2048, 128), BF),
            pltpu.VMEM((16, 80, 2048), BF),
            pltpu.VMEM((16, 128, 128), BF),
            pltpu.VMEM((8, 128, 128), BF),
            pltpu.VMEM((256, 128), F32),
            pltpu.VMEM((256, 128), F32),
            dma((6,)),
            dma((4, 8 * PXY)),
            dma((4, 8 * PXY)),
            dma((2, 16)),
            dma((2, 16)),
            dma((2, 8 * (PZ + 1))),
            dma((2, 8 * (PZ + 1))),
            dma((1,)),
            dma((1,)),
            dma((1,)),
            dma((1,)),
            dma((8,)),
            dma((8,)),
        ],
        compiler_params=pltpu.CompilerParams(
            collective_id=0, has_side_effects=True, vmem_limit_bytes=60 * 1024 * 1024
        ),
        name="latent_attention",
    )(
        ql, kl, rk, qg.reshape(1, -1), kg.reshape(1, -1),
        *(jnp.asarray(t) for t in rotary_tables()),
        nq, bq, nk, nv, bk, bv,
    )


def solution(mesh):
    in_specs = (
        P("dp", "sp", None),
        P("dp", "sp", None),
        P("dp", "sp", None),
        P(),
        P(),
        P("dp", None),
        P("dp", None),
        P("dp", None),
        P("dp", None),
        P("dp", None),
        P("dp", None),
    )
    out_specs = (P("dp", "sp", None), P("dp", "sp", None))
    return jax.shard_map(
        on_device, mesh=mesh, in_specs=in_specs, out_specs=out_specs, check_vma=False
    )
```

```python
import functools
import math

import jax
import jax.numpy as jnp
import numpy as np
from jax import lax
from jax.experimental import pallas as pl
from jax.experimental.pallas import tpu as pltpu
from jax.sharding import PartitionSpec as P

EPSILON = 1e-06
ROTARY_BASE = 10000.0
PZ = 4
Z_EARLY = 4
HOOK = 4
BF = jnp.bfloat16
F32 = jnp.float32
MESH = pl.DeviceIdType.MESH
NARROW_SCALE = 96 ** -0.5 * math.log2(math.e)
BROAD_SCALE = 160 ** -0.5 * math.log2(math.e)


def rotary_tables():
    frequency = ROTARY_BASE ** (-np.arange(16, dtype=np.float64) / 16)
    lanes = np.tile(frequency, 8)
    coarse = (256.0 * np.arange(8))[:, None] * lanes[None, :]
    fine = np.arange(256.0)[:, None] * lanes[None, :]
    return tuple(
        np.asarray(t, np.float32)
        for t in (np.cos(coarse), np.sin(coarse), np.cos(fine), np.sin(fine))
    )


def lane_iota(shape):
    return lax.broadcasted_iota(jnp.int32, shape, len(shape) - 1)


def row_iota(shape):
    return lax.broadcasted_iota(jnp.int32, shape, 0)


def normalize(latent, gain_row):
    values = latent.astype(F32)
    scaled = values * lax.rsqrt(jnp.mean(values * values, axis=-1, keepdims=True) + EPSILON)
    return (scaled * gain_row).astype(BF)


def rotate(values, cosine, signed_sine):
    first = lane_iota(values.shape) % 32 < 16
    swapped = jnp.where(first, pltpu.roll(values, 112, 1), pltpu.roll(values, 16, 1))
    return values * cosine + swapped * signed_sine


def take(columns, segments):
    rows = columns.shape[0]
    lane = lane_iota((rows, 128))
    out, dest = None, 0
    for start, width in segments:
        tile, off = start // 128, start % 128
        span = 128 if off + width <= 128 else 256
        window = columns[:, tile * 128 : tile * 128 + span]
        shift = (dest - off) % span
        moved = pltpu.roll(window, shift, 1)[:, :128] if shift else window[:, :128]
        out = moved if out is None else jnp.where(lane >= dest, moved, out)
        dest += width
    return out


def body(
    ql, kl, rk, qg, kg, ca, sa, cb, sb, nq, bq, nk, nv, bk, bv,
    out_n, out_b,
    raw_n, raw_b, wq8, wkv, kv, rt, qn, wq, wvt, qmt, kp, kr, vt, at, sbuf, cos_t, sin_t,
    s_buf, p_buf, acc_buf, top_buf,
    in_sem, f_send, f_recv, g_send, g_recv, dd_send, dd_recv, z_send, z_recv,
    q_send, q_recv, o_send, o_recv,
):
    z = lax.axis_index("sp")
    d = lax.axis_index("dp")
    par = lax.rem(z, 2)
    core = lax.rem(d, 2)
    chip = d // 2
    here = (lax.rem(chip, 4), chip // 4)
    partner_core = d + 1 - 2 * core
    mate = z + 1 - 2 * par
    zs = {k: lax.rem(z + k + 16, 16) for k in range(-8, 9)}

    where = {}
    for t in range(2):
        along = [[lax.rem(here[axis] + k, 4) for k in range(4)] for axis in (t, 1 - t)]
        for a in range(4):
            for b in range(4):
                xy = (along[0][a], along[1][b]) if t == 0 else (along[1][b], along[0][a])
                where[t, a, b] = (xy[1] * 4 + xy[0]) * 2 + core

    def cols(ref, width):
        return ref.at[:, pl.ds(pl.multiple_of(par * width, 128), width)]

    own_rows = pl.ds(pl.multiple_of(d * 16, 16), 16)
    loads = [
        pltpu.make_async_copy(cols(nq, 768), raw_n, in_sem.at[0]),
        pltpu.make_async_copy(cols(bq, 1280), raw_b, in_sem.at[1]),
        pltpu.make_async_copy(cols(nk, 512), wkv.at[own_rows, pl.ds(0, 512)], in_sem.at[2]),
        pltpu.make_async_copy(cols(bk, 1024), wkv.at[own_rows, pl.ds(512, 1024)], in_sem.at[3]),
        pltpu.make_async_copy(cols(nv, 512), wkv.at[own_rows, pl.ds(1536, 512)], in_sem.at[4]),
        pltpu.make_async_copy(cols(bv, 512), wkv.at[own_rows, pl.ds(2048, 512)], in_sem.at[5]),
    ]
    for load in loads:
        load.start()

    barrier = pltpu.get_barrier_semaphore()
    near = [{"sp": zs[1]}, {"sp": zs[-1]}, {"dp": partner_core}]
    near += [{"dp": where[t, k, 0]} for t in range(2) for k in (1, 3)]
    for who in near:
        pl.semaphore_signal(barrier, inc=1, device_id=who, device_id_type=MESH)

    kv[z] = normalize(kl[0], kg[...])
    half = pl.ds(pl.multiple_of(par * 128, 128), 128)
    coarse = pl.ds(z // 2, 1)
    cosine = ca[coarse, :] * cb[...] - sa[coarse, :] * sb[...]
    sine = sa[coarse, :] * cb[...] + ca[coarse, :] * sb[...]
    cos_t[...] = cosine
    sin_t[...] = jnp.where(lane_iota(sine.shape) % 32 < 16, -sine, sine)
    own_rope = rk[0].astype(F32)
    rope4 = jnp.concatenate([own_rope] * 4, axis=0).T
    rope4 = rotate(rope4, cos_t[half, :], sin_t[half, :])
    rt[z] = rope4.T[:32].astype(BF)
    qn[par] = normalize(ql[0], qg[...])
    for load in loads:
        load.wait()
    wn, wb = raw_n[...].astype(F32), raw_b[...].astype(F32)
    blocks = [take(wn, [(192 * j, 64), (192 * j + 96, 64)]) for j in range(4)]
    blocks += [take(wb, [(160 * h, 128)]) for h in range(8)]
    blocks += [take(wn, [(96 * h + 64, 32) for h in range(4 * g, 4 * g + 4)]) for g in range(2)]
    blocks += [take(wb, [(160 * h + 128, 32) for h in range(4 * g, 4 * g + 4)]) for g in range(2)]
    for i, block in enumerate(blocks):
        for t in range(3):
            wq8[3 * d + t, :, 128 * i : 128 * i + 128] = block[8 * t : 8 * t + 8].astype(BF)

    pl.semaphore_wait(barrier, 7)

    started = []

    def start(make):
        make().start()
        started.append(make)

    def piece(t, slot, h):
        if t == 0:
            return wq8.at[pl.ds(3 * slot, 3), :, pl.ds(h * 1024, 1024)]
        return wkv.at[pl.ds(pl.multiple_of(16 * slot, 16), 16), pl.ds(h * 1280, 1280)]

    def xy_desc(t, a, b, h, send, recv, to):
        ref = piece(t, where[t, a, b], h)
        return pltpu.make_async_remote_copy(
            ref, ref, send, recv, device_id={"dp": to}, device_id_type=MESH
        )

    def f_send_copy(t, a, h, to):
        named = (a - to) % 4
        index = (t * 4 + named) * 2 + h
        return lambda: xy_desc(
            t, a, 0, h, f_send.at[index], f_recv.at[index], where[t, to % 4, 0]
        )

    def g_send_copy(t, a, b, h, to):
        named = (b - to) % 4
        index = ((t * 4 + a) * 4 + named) * 2 + h
        return lambda: xy_desc(
            t, a, b, h, g_send.at[index], g_recv.at[index], where[t, 0, to % 4]
        )

    def d_copy(t, a, b, h):
        index = ((t * 4 + a) * 4 + b) * 2 + h
        return lambda: xy_desc(
            t, a, b, h, dd_send.at[index], dd_recv.at[index], partner_core
        )

    def column(t, a, h):
        for to in (1, -1):
            start(g_send_copy(t, a, 0, h, to))
        start(d_copy(t, a, 0, h))

    def f_event(t, a, h):
        index = (t * 4 + a) * 2 + h
        xy_desc(t, a, 0, h, f_send.at[index], f_recv.at[index], d).wait_recv()
        if (a, h) == (3, 0):
            start(f_send_copy(t, a, h, 1))
        if (a, h) == (1, 1):
            start(f_send_copy(t, a, h, -1))
        column(t, a, h)

    def g_event(t, a, b, h):
        index = ((t * 4 + a) * 4 + b) * 2 + h
        xy_desc(t, a, b, h, g_send.at[index], g_recv.at[index], d).wait_recv()
        if (b, h) == (3, 0):
            start(g_send_copy(t, a, b, h, 1))
        if (b, h) == (1, 1):
            start(g_send_copy(t, a, b, h, -1))
        start(d_copy(t, a, b, h))

    rows_z = 128 // PZ

    def z_desc(way, step, i, slot):
        ref = rt.at[slot] if i == PZ else kv.at[slot, pl.ds(i * rows_z, rows_z)]
        index = (step - 1) * (PZ + 1) + i
        return pltpu.make_async_remote_copy(
            ref, ref, z_send.at[way, index], z_recv.at[way, index],
            device_id={"sp": zs[1 - 2 * way]}, device_id_type=MESH,
        )

    def z_copy(way, step, i):
        return lambda: z_desc(way, step, i, zs[-(1 - 2 * way) * (step - 1)])

    def z_pieces(way, step):
        if step < 8:
            return [PZ] + list(range(PZ))
        return [PZ] + list(range(PZ // 2)) if way == 0 else list(range(PZ // 2, PZ))

    def z_event(step, i):
        for way in range(2):
            if i not in z_pieces(way, step):
                continue
            z_desc(way, step, i, zs[-(1 - 2 * way) * step]).wait_recv()
            if step < 8 and i in z_pieces(way, step + 1):
                start(z_copy(way, step + 1, i))

    def z_step(step):
        for i in z_pieces(0, 1):
            z_event(step, i)

    for h in range(2):
        for t in (1, 0):
            for to in (1, -1):
                start(f_send_copy(t, 0, h, to))
    for i in z_pieces(0, 1):
        for way in range(2):
            start(z_copy(way, 1, i))
    for h in range(2):
        for t in (1, 0):
            column(t, 0, h)
    mine = qn.at[par]
    start(
        lambda: pltpu.make_async_remote_copy(
            mine, mine, q_send.at[0], q_recv.at[0], device_id={"sp": mate}, device_id_type=MESH
        )
    )

    events = []
    for t in (1, 0):
        for h in range(2):
            for a in (1, 3):
                events.append((3.0 + h, f_event, (t, a, h)))
            events.append((6.0 + h, f_event, (t, 2, h)))
            for b in (1, 3):
                events.append((5.0 + h, g_event, (t, 0, b, h)))
                events.append((8.0 + h, g_event, (t, 1, b, h)))
                events.append((10.0 + h, g_event, (t, 3, b, h)))
                events.append((13.0 + h, g_event, (t, 2, b, h)))
            events.append((8.5 + h, g_event, (t, 0, 2, h)))
            events.append((11.5 + h, g_event, (t, 1, 2, h)))
            events.append((13.5 + h, g_event, (t, 3, 2, h)))
            events.append((16.5 + h, g_event, (t, 2, 2, h)))
    for step in range(1, Z_EARLY + 1):
        for k, i in enumerate(z_pieces(0, 1)):
            events.append((3.7 * step - 2 + 0.5 * k, z_event, (step, i)))
    for _, event, what in sorted(events, key=lambda e: e[0]):
        event(*what)
    for t in (1, 0):
        for a in range(4):
            for b in range(4):
                for h in range(2):
                    index = ((t * 4 + a) * 4 + b) * 2 + h
                    ref = piece(t, where[t, a, b] + 1 - 2 * core, h)
                    pltpu.make_async_remote_copy(
                        ref, ref, dd_send.at[index], dd_recv.at[index],
                        device_id={"dp": partner_core}, device_id_type=MESH,
                    ).wait_recv()
    theirs = qn.at[1 - par]
    pltpu.make_async_remote_copy(
        theirs, theirs, q_send.at[0], q_recv.at[0], device_id={"sp": mate}, device_id_type=MESH
    ).wait_recv()

    def pack_rows(g, carry):
        pair = jnp.concatenate([wq8[2 * g].astype(F32), wq8[2 * g + 1].astype(F32)], axis=0)
        wq[pl.ds(pl.multiple_of(16 * g, 16), 16), :] = pair.astype(BF)
        return carry

    lax.fori_loop(0, 48, pack_rows, 0)
    for i in range(8):
        wvt[128 * i : 128 * i + 128, :] = wkv[:, 1536 + 128 * i : 1664 + 128 * i].T

    tokens = jnp.concatenate([qn[0], qn[1]], axis=0)
    group = row_iota((128, 256)) // 32
    side = row_iota((128, 256)) // 64
    nothing = jnp.zeros((128, 256), BF)
    for pair in range(8):
        both = jnp.dot(tokens, wq[:, 256 * pair : 256 * pair + 256], preferred_element_type=F32)
        for k in range(2):
            block = 2 * pair + k
            part = both[:, 128 * k : 128 * k + 128]
            if block >= 12:
                part = rotate(part, cos_t[...], sin_t[...])
            turned = part.astype(BF).T
            if block < 4:
                for s in range(2):
                    qmt[2 * block + s, 0:128, :] = jnp.where(side == s, turned, nothing)
            elif block < 12:
                qmt[block + 4, 0:128, :] = turned
            else:
                for g in range(4):
                    head = 4 * (block - 12) + g
                    qmt[head, 128:256, :] = jnp.where(group == g, turned, nothing)

    for h in range(16):
        vt[h, 64:80, :] = jnp.ones((16, 2048), BF)

    def project(b, one, two):
        rows = pl.ds(pl.multiple_of(256 * b, 256), 256)
        x = jnp.concatenate([kv[one], kv[two]], axis=0)
        for i in range(6):
            kp[rows, 256 * i : 256 * i + 256] = jnp.dot(
                x, wkv[:, 256 * i : 256 * i + 256], preferred_element_type=F32
            ).astype(BF)
        for i in range(4):
            turned = lax.dot_general(
                wvt[256 * i : 256 * i + 256, :], x, (((1,), (1,)), ((), ())),
                preferred_element_type=F32,
            ).astype(BF)
            for k in range(4):
                vt[4 * i + k, 0:64, rows] = turned[64 * k : 64 * k + 64]
        for k, slot in enumerate((one, two)):
            own = rt[slot].astype(F32)
            kr[pl.ds(pl.multiple_of(256 * b + 128 * k, 128), 128), :] = (
                jnp.concatenate([own, own, own, own], axis=0).T.astype(BF)
            )

    def project_steps(first, last):
        def one_step(s, carry):
            project(s - 1, lax.rem(z + 16 - s, 16), lax.rem(z + lax.rem(s, 8) + 16, 16))
            return carry

        lax.fori_loop(first, last + 1, one_step, 0)

    def out_desc(j):
        broad = j // 4
        dst = 8 * broad + 4 * par + j - 4 * broad
        return pltpu.make_async_remote_copy(
            sbuf.at[j], at.at[dst], o_send.at[j], o_recv.at[j],
            device_id={"sp": mate}, device_id_type=MESH,
        )

    def finish_pair(j, parts):
        broad = j // 4
        stacked = jnp.concatenate(parts, axis=0).astype(BF)
        low, high = stacked[:, 0:128].T, stacked[:, 128:256].T
        even = par == 0
        at[8 * broad + 4 * par + j - 4 * broad] = jnp.where(even, low, high)
        sbuf[j] = jnp.where(even, high, low)
        out_desc(j).start()

    def factor_of(h):
        return jnp.where(h < 8, NARROW_SCALE, BROAD_SCALE).astype(F32)

    def attention(block0, count, last, hook):
        def rows_of(b):
            return slice((block0 + b) * 256, (block0 + b) * 256 + 256)

        def here_of(b):
            return slice(b * 256, b * 256 + 256)

        def score(h, slot, b):
            broad = h // 8
            block = (1 - broad) * (h // 2) + broad * (h - 4)
            lanes = pl.ds(pl.multiple_of(block * 128, 128), 128)
            keys = jnp.concatenate([kp[rows_of(b), lanes], kr[rows_of(b), :]], axis=1)
            scores = jnp.dot(keys, qmt[h], preferred_element_type=F32)
            s_buf[slot, here_of(b), :] = scores
            return jnp.max(scores.reshape(32, 8, 256), axis=0)

        def settle(h, peak):
            top = jnp.max(peak, axis=0, keepdims=True)
            if last:
                top = jnp.maximum(top, top_buf[0, h])
            top_buf[int(last), h] = top
            return top

        def soften(slot, b, top, factor):
            p_buf[slot, here_of(b), :] = jnp.exp2(
                (s_buf[slot, here_of(b), :] - top) * factor
            ).astype(BF)

        def gather(h, slot):
            keys = slice(block0 * 256, (block0 + count) * 256)
            return jnp.dot(
                vt[h, :, keys], p_buf[slot, : count * 256, :], preferred_element_type=F32
            )

        def all_scores(h, slot):
            peak = score(h, slot, 0)
            for b in range(1, count):
                peak = jnp.maximum(peak, score(h, slot, b))
            return settle(h, peak)

        first_top = all_scores(0, 0)
        for b in range(count):
            soften(0, b, first_top, factor_of(0))
        second_top = all_scores(1, 1)

        def step(i, top):
            hook(i)
            parts = []
            for k in range(2):
                h = 2 * i + k
                ahead = jnp.minimum(h + 2, 15)
                factor = factor_of(jnp.minimum(h + 1, 15))
                sums = gather(h, k)
                peak = None
                for b in range(count):
                    found = score(ahead, k, b)
                    peak = found if peak is None else jnp.maximum(peak, found)
                    soften(1 - k, b, top, factor)
                if last:
                    kept = jnp.exp2((top_buf[0, h] - top_buf[1, h]) * factor_of(h))
                    whole = acc_buf[h] * kept + sums
                    parts.append(whole[0:64] / whole[64:65])
                else:
                    acc_buf[h] = sums
                top = settle(ahead, peak)
            if last:
                finish_pair(i, parts)
            return top

        lax.fori_loop(0, 8, step, second_top)

    for step in range(Z_EARLY + 1, 6):
        z_step(step)
    project_steps(1, 5)
    z_step(6)

    def hook(i):
        @pl.when(i == HOOK)
        def _():
            z_step(7)

    attention(0, 5, False, hook)
    z_step(8)
    project_steps(6, 8)
    attention(5, 3, True, lambda i: None)

    def landed(j, carry):
        broad = j // 4
        src = 8 * broad + 4 * (1 - par) + j - 4 * broad
        pltpu.make_async_remote_copy(
            at.at[src], at.at[src], o_send.at[j], o_recv.at[j],
            device_id={"sp": mate}, device_id_type=MESH,
        ).wait_recv()
        out_desc(j).wait_send()
        return carry

    lax.fori_loop(0, 8, landed, 0)
    for which, out in enumerate((out_n, out_b)):
        values = [at[8 * which + i].astype(F32) for i in range(8)]
        squares = sum(v * v for v in values)
        mean = jnp.sum(squares, axis=-1, keepdims=True) * (1.0 / 1024)
        scale = lax.rsqrt(mean + EPSILON)
        for i in range(8):
            out[0, :, 128 * i : 128 * i + 128] = (values[i] * scale).astype(BF)

    for make in started:
        make().wait_send()


def on_device(ql, kl, rk, qg, kg, nq, bq, nk, nv, bk, bv):
    vmem = pl.BlockSpec(memory_space=pltpu.VMEM)
    hbm = pl.BlockSpec(memory_space=pl.ANY)
    dma = pltpu.SemaphoreType.DMA
    return pl.pallas_call(
        body,
        out_shape=[jax.ShapeDtypeStruct((1, 128, 1024), BF)] * 2,
        in_specs=[vmem] * 9 + [hbm] * 6,
        out_specs=[vmem] * 2,
        scratch_shapes=[
            pltpu.VMEM((24, 768), BF),
            pltpu.VMEM((24, 1280), BF),
            pltpu.VMEM((96, 8, 2048), BF),
            pltpu.VMEM((512, 2560), BF),
            pltpu.VMEM((16, 128, 512), BF),
            pltpu.VMEM((16, 32, 128), BF),
            pltpu.VMEM((2, 128, 768), BF),
            pltpu.VMEM((768, 2048), BF),
            pltpu.VMEM((1024, 512), BF),
            pltpu.VMEM((16, 256, 256), BF),
            pltpu.VMEM((2048, 1536), BF),
            pltpu.VMEM((2048, 128), BF),
            pltpu.VMEM((16, 80, 2048), BF),
            pltpu.VMEM((16, 128, 128), BF),
            pltpu.VMEM((8, 128, 128), BF),
            pltpu.VMEM((256, 128), F32),
            pltpu.VMEM((256, 128), F32),
            pltpu.VMEM((2, 1280, 256), F32),
            pltpu.VMEM((2, 1280, 256), BF),
            pltpu.VMEM((16, 80, 256), F32),
            pltpu.VMEM((2, 16, 1, 256), F32),
            dma((6,)),
            dma((16,)),
            dma((16,)),
            dma((64,)),
            dma((64,)),
            dma((64,)),
            dma((64,)),
            dma((2, 8 * (PZ + 1))),
            dma((2, 8 * (PZ + 1))),
            dma((1,)),
            dma((1,)),
            dma((8,)),
            dma((8,)),
        ],
        compiler_params=pltpu.CompilerParams(
            collective_id=0, has_side_effects=True, vmem_limit_bytes=60 * 1024 * 1024
        ),
        name="latent_attention",
    )(
        ql, kl, jnp.swapaxes(rk, 1, 2), qg.reshape(1, -1), kg.reshape(1, -1),
        *(jnp.asarray(t) for t in rotary_tables()),
        nq, bq, nk, nv, bk, bv,
    )


def solution(mesh):
    in_specs = (
        P("dp", "sp", None),
        P("dp", "sp", None),
        P("dp", "sp", None),
        P(),
        P(),
        P("dp", None),
        P("dp", None),
        P("dp", None),
        P("dp", None),
        P("dp", None),
        P("dp", None),
    )
    out_specs = (P("dp", "sp", None), P("dp", "sp", None))
    return jax.shard_map(
        on_device, mesh=mesh, in_specs=in_specs, out_specs=out_specs, check_vma=False
    )
```

```python
import functools
import math

import jax
import jax.numpy as jnp
import numpy as np
from jax import lax
from jax.experimental import pallas as pl
from jax.experimental.pallas import tpu as pltpu
from jax.sharding import PartitionSpec as P

EPSILON = 1e-06
ROTARY_BASE = 10000.0
PZ = 4
Z_EARLY = 4
HOOK = 4
VMEM_LIMIT = 60 * 1024 * 1024
BF = jnp.bfloat16
F32 = jnp.float32
MESH = pl.DeviceIdType.MESH
NARROW_SCALE = 96 ** -0.5 * math.log2(math.e)
BROAD_SCALE = 160 ** -0.5 * math.log2(math.e)


def rotary_tables():
    frequency = ROTARY_BASE ** (-np.arange(16, dtype=np.float64) / 16)
    lanes = np.tile(frequency, 8)
    coarse = (256.0 * np.arange(8))[:, None] * lanes[None, :]
    fine = np.arange(256.0)[:, None] * lanes[None, :]
    return tuple(
        np.asarray(t, np.float32)
        for t in (np.cos(coarse), np.sin(coarse), np.cos(fine), np.sin(fine))
    )


def lane_iota(shape):
    return lax.broadcasted_iota(jnp.int32, shape, len(shape) - 1)


def row_iota(shape):
    return lax.broadcasted_iota(jnp.int32, shape, 0)


def normalize(latent, gain_row):
    values = latent.astype(F32)
    scaled = values * lax.rsqrt(jnp.mean(values * values, axis=-1, keepdims=True) + EPSILON)
    return (scaled * gain_row[None, :]).astype(BF)


def rotate(values, cosine, signed_sine):
    first = lane_iota(values.shape) % 32 < 16
    swapped = jnp.where(first, pltpu.roll(values, 112, 1), pltpu.roll(values, 16, 1))
    return values * cosine + swapped * signed_sine


def take(columns, segments):
    rows = columns.shape[0]
    lane = lane_iota((rows, 128))
    out, dest = None, 0
    for start, width in segments:
        tile, off = start // 128, start % 128
        span = 128 if off + width <= 128 else 256
        window = columns[:, tile * 128 : tile * 128 + span]
        shift = (dest - off) % span
        moved = pltpu.roll(window, shift, 1)[:, :128] if shift else window[:, :128]
        out = moved if out is None else jnp.where(lane >= dest, moved, out)
        dest += width
    return out


def body(
    ql, kl, rk, qg, kg, ca, sa, cb, sb, nq, bq, nk, nv, bk, bv,
    out_n, out_b,
    raw_n, raw_b, wq8, wkv, kv, rt, qn, wq, wvt, qmt, kp, kr, vt, at, sbuf, cos_t, sin_t,
    s_buf, p_buf, acc_buf, top_buf,
    v_ql, v_kl, v_rk, v_qg, v_kg, v_ca, v_sa, v_cb, v_sb,
    in_sem, f_send, f_recv, g_send, g_recv, dd_send, dd_recv, z_send, z_recv,
    q_send, q_recv, o_send, o_recv,
):
    z = lax.axis_index("sp")
    d = lax.axis_index("dp")
    par = lax.rem(z, 2)
    core = lax.rem(d, 2)
    chip = d // 2
    here = (lax.rem(chip, 4), chip // 4)
    partner_core = d + 1 - 2 * core
    mate = z + 1 - 2 * par
    zs = {k: lax.rem(z + k + 16, 16) for k in range(-8, 9)}

    where = {}
    for t in range(2):
        along = [[lax.rem(here[axis] + k, 4) for k in range(4)] for axis in (t, 1 - t)]
        for a in range(4):
            for b in range(4):
                xy = (along[0][a], along[1][b]) if t == 0 else (along[1][b], along[0][a])
                where[t, a, b] = (xy[1] * 4 + xy[0]) * 2 + core

    def cols(ref, width):
        return ref.at[:, pl.ds(pl.multiple_of(par * width, 128), width)]

    barrier = pltpu.get_barrier_semaphore()
    near = [{"sp": zs[1]}, {"sp": zs[-1]}, {"dp": partner_core}]
    near += [{"dp": where[t, k, 0]} for t in range(2) for k in (1, 3)]
    for who in near:
        pl.semaphore_signal(barrier, inc=1, device_id=who, device_id_type=MESH)

    own_rows = pl.ds(pl.multiple_of(d * 16, 16), 16)
    pairs = [
        (cols(nk, 512), wkv.at[own_rows, pl.ds(0, 512)]),
        (cols(bk, 1024), wkv.at[own_rows, pl.ds(512, 1024)]),
        (cols(nv, 512), wkv.at[own_rows, pl.ds(1536, 512)]),
        (cols(bv, 512), wkv.at[own_rows, pl.ds(2048, 512)]),
        (cols(nq, 768), raw_n),
        (cols(bq, 1280), raw_b),
        (kl, v_kl), (kg, v_kg), (rk, v_rk), (ca, v_ca), (sa, v_sa), (cb, v_cb), (sb, v_sb),
        (ql, v_ql), (qg, v_qg),
    ]
    loads = [
        pltpu.make_async_copy(src, dst, in_sem.at[i]) for i, (src, dst) in enumerate(pairs)
    ]
    for load in loads:
        load.start()

    def arrange_columns():
        wn, wb = raw_n[...].astype(F32), raw_b[...].astype(F32)
        blocks = [take(wn, [(192 * j, 64), (192 * j + 96, 64)]) for j in range(4)]
        blocks += [take(wb, [(160 * h, 128)]) for h in range(8)]
        for w, size in ((wn, 96), (wb, 160)):
            for g in range(0, 8, 4):
                pieces = [(size * h + size - 32, 32) for h in range(g, g + 4)]
                blocks.append(take(w, pieces))
        for i, block in enumerate(blocks):
            for t in range(3):
                wq8[3 * d + t, :, 128 * i : 128 * i + 128] = block[8 * t : 8 * t + 8].astype(BF)

    def own_pair():
        kv[z] = normalize(v_kl[0], v_kg[...])
        half = pl.ds(pl.multiple_of(par * 128, 128), 128)
        coarse = pl.ds(z // 2, 1)
        cosine = v_ca[coarse, :] * v_cb[...] - v_sa[coarse, :] * v_sb[...]
        sine = v_sa[coarse, :] * v_cb[...] + v_ca[coarse, :] * v_sb[...]
        cos_t[...] = cosine
        sin_t[...] = jnp.where(lane_iota(sine.shape) % 32 < 16, -sine, sine)
        own_rope = v_rk[0].astype(F32)
        rope4 = jnp.concatenate([own_rope] * 4, axis=0).T
        rope4 = rotate(rope4, cos_t[half, :], sin_t[half, :])
        rt[z] = rope4.T[:32].astype(BF)

    started = []

    def start(make):
        make().start()
        started.append(make)

    def piece(t, slot, h):
        if t == 0:
            return wq8.at[pl.ds(3 * slot, 3), :, pl.ds(h * 1024, 1024)]
        return wkv.at[pl.ds(pl.multiple_of(16 * slot, 16), 16), pl.ds(h * 1280, 1280)]

    def xy_desc(t, a, b, h, send, recv, to):
        ref = piece(t, where[t, a, b], h)
        return pltpu.make_async_remote_copy(
            ref, ref, send, recv, device_id={"dp": to}, device_id_type=MESH
        )

    def f_send_copy(t, a, h, to):
        named = (a - to) % 4
        index = (t * 4 + named) * 2 + h
        return lambda: xy_desc(
            t, a, 0, h, f_send.at[index], f_recv.at[index], where[t, to % 4, 0]
        )

    def g_send_copy(t, a, b, h, to):
        named = (b - to) % 4
        index = ((t * 4 + a) * 4 + named) * 2 + h
        return lambda: xy_desc(
            t, a, b, h, g_send.at[index], g_recv.at[index], where[t, 0, to % 4]
        )

    def d_copy(t, a, b, h):
        index = ((t * 4 + a) * 4 + b) * 2 + h
        return lambda: xy_desc(
            t, a, b, h, dd_send.at[index], dd_recv.at[index], partner_core
        )

    def column(t, a, h):
        for to in (1, -1):
            start(g_send_copy(t, a, 0, h, to))
        start(d_copy(t, a, 0, h))

    def f_event(t, a, h):
        index = (t * 4 + a) * 2 + h
        xy_desc(t, a, 0, h, f_send.at[index], f_recv.at[index], d).wait_recv()
        if (a, h) == (3, 0):
            start(f_send_copy(t, a, h, 1))
        if (a, h) == (1, 1):
            start(f_send_copy(t, a, h, -1))
        column(t, a, h)

    def g_event(t, a, b, h):
        index = ((t * 4 + a) * 4 + b) * 2 + h
        xy_desc(t, a, b, h, g_send.at[index], g_recv.at[index], d).wait_recv()
        if (b, h) == (3, 0):
            start(g_send_copy(t, a, b, h, 1))
        if (b, h) == (1, 1):
            start(g_send_copy(t, a, b, h, -1))
        start(d_copy(t, a, b, h))

    rows_z = 128 // PZ

    def z_desc(way, step, i, slot):
        ref = rt.at[slot] if i == PZ else kv.at[slot, pl.ds(i * rows_z, rows_z)]
        index = (step - 1) * (PZ + 1) + i
        return pltpu.make_async_remote_copy(
            ref, ref, z_send.at[way, index], z_recv.at[way, index],
            device_id={"sp": zs[1 - 2 * way]}, device_id_type=MESH,
        )

    def z_copy(way, step, i):
        return lambda: z_desc(way, step, i, zs[-(1 - 2 * way) * (step - 1)])

    def z_pieces(way, step):
        if step < 8:
            return [PZ] + list(range(PZ))
        return [PZ] + list(range(PZ // 2)) if way == 0 else list(range(PZ // 2, PZ))

    def z_event(step, i):
        for way in range(2):
            if i not in z_pieces(way, step):
                continue
            z_desc(way, step, i, zs[-(1 - 2 * way) * step]).wait_recv()
            if step < 8 and i in z_pieces(way, step + 1):
                start(z_copy(way, step + 1, i))

    def z_step(step):
        for i in z_pieces(0, 1):
            z_event(step, i)

    def send_weights(t):
        for h in range(2):
            for to in (1, -1):
                start(f_send_copy(t, 0, h, to))
        for h in range(2):
            column(t, 0, h)

    for load in loads[:4]:
        load.wait()
    pl.semaphore_wait(barrier, 7)
    send_weights(1)
    for load in loads[4:6]:
        load.wait()
    arrange_columns()
    for load in loads[6:13]:
        load.wait()
    own_pair()
    send_weights(0)
    for load in loads[13:]:
        load.wait()
    qn[par] = normalize(v_ql[0], v_qg[...])
    for i in z_pieces(0, 1):
        for way in range(2):
            start(z_copy(way, 1, i))
    for h in range(16):
        vt[h, 64:80, :] = jnp.ones((16, 2048), BF)
    mine = qn.at[par]
    start(
        lambda: pltpu.make_async_remote_copy(
            mine, mine, q_send.at[0], q_recv.at[0], device_id={"sp": mate}, device_id_type=MESH
        )
    )

    events = []
    for t in (1, 0):
        for h in range(2):
            for a in (1, 3):
                events.append((3.0 + h, f_event, (t, a, h)))
            events.append((6.0 + h, f_event, (t, 2, h)))
            for b in (1, 3):
                events.append((5.0 + h, g_event, (t, 0, b, h)))
                events.append((8.0 + h, g_event, (t, 1, b, h)))
                events.append((10.0 + h, g_event, (t, 3, b, h)))
                events.append((13.0 + h, g_event, (t, 2, b, h)))
            events.append((8.5 + h, g_event, (t, 0, 2, h)))
            events.append((11.5 + h, g_event, (t, 1, 2, h)))
            events.append((13.5 + h, g_event, (t, 3, 2, h)))
            events.append((16.5 + h, g_event, (t, 2, 2, h)))
    for step in range(1, Z_EARLY + 1):
        for k, i in enumerate(z_pieces(0, 1)):
            events.append((3.7 * step - 2 + 0.5 * k, z_event, (step, i)))
    for _, event, what in sorted(events, key=lambda e: e[0]):
        event(*what)
    for t in (1, 0):
        for a in range(4):
            for b in range(4):
                for h in range(2):
                    index = ((t * 4 + a) * 4 + b) * 2 + h
                    ref = piece(t, where[t, a, b] + 1 - 2 * core, h)
                    pltpu.make_async_remote_copy(
                        ref, ref, dd_send.at[index], dd_recv.at[index],
                        device_id={"dp": partner_core}, device_id_type=MESH,
                    ).wait_recv()
    theirs = qn.at[1 - par]
    pltpu.make_async_remote_copy(
        theirs, theirs, q_send.at[0], q_recv.at[0], device_id={"sp": mate}, device_id_type=MESH
    ).wait_recv()

    def pack_rows(g, carry):
        pair = jnp.concatenate([wq8[2 * g].astype(F32), wq8[2 * g + 1].astype(F32)], axis=0)
        wq[pl.ds(pl.multiple_of(16 * g, 16), 16), :] = pair.astype(BF)
        return carry

    lax.fori_loop(0, 48, pack_rows, 0)
    for i in range(8):
        wvt[128 * i : 128 * i + 128, :] = wkv[:, 1536 + 128 * i : 1664 + 128 * i].T

    tokens = jnp.concatenate([qn[0], qn[1]], axis=0)
    group = row_iota((128, 256)) // 32
    side = row_iota((128, 256)) // 64
    nothing = jnp.zeros((128, 256), BF)
    for pair in range(8):
        both = jnp.dot(tokens, wq[:, 256 * pair : 256 * pair + 256], preferred_element_type=F32)
        for k in range(2):
            block = 2 * pair + k
            part = both[:, 128 * k : 128 * k + 128]
            if block >= 12:
                part = rotate(part, cos_t[...], sin_t[...])
            turned = part.astype(BF).T
            if block < 4:
                for s in range(2):
                    qmt[2 * block + s, 0:128, :] = jnp.where(side == s, turned, nothing)
            elif block < 12:
                qmt[block + 4, 0:128, :] = turned
            else:
                for g in range(4):
                    head = 4 * (block - 12) + g
                    qmt[head, 128:256, :] = jnp.where(group == g, turned, nothing)

    def project(b, one, two):
        rows = pl.ds(pl.multiple_of(256 * b, 256), 256)
        x = jnp.concatenate([kv[one], kv[two]], axis=0)
        for i in range(6):
            kp[rows, 256 * i : 256 * i + 256] = jnp.dot(
                x, wkv[:, 256 * i : 256 * i + 256], preferred_element_type=F32
            ).astype(BF)
        for i in range(4):
            turned = lax.dot_general(
                wvt[256 * i : 256 * i + 256, :], x, (((1,), (1,)), ((), ())),
                preferred_element_type=F32,
            ).astype(BF)
            for k in range(4):
                vt[4 * i + k, 0:64, rows] = turned[64 * k : 64 * k + 64]
        for k, slot in enumerate((one, two)):
            own = rt[slot].astype(F32)
            kr[pl.ds(pl.multiple_of(256 * b + 128 * k, 128), 128), :] = (
                jnp.concatenate([own, own, own, own], axis=0).T.astype(BF)
            )

    def project_steps(first, last):
        def one_step(s, carry):
            project(s - 1, lax.rem(z + 16 - s, 16), lax.rem(z + lax.rem(s, 8) + 16, 16))
            return carry

        lax.fori_loop(first, last + 1, one_step, 0)

    def out_desc(j):
        broad = j // 4
        dst = 8 * broad + 4 * par + j - 4 * broad
        return pltpu.make_async_remote_copy(
            sbuf.at[j], at.at[dst], o_send.at[j], o_recv.at[j],
            device_id={"sp": mate}, device_id_type=MESH,
        )

    def finish_pair(j, parts):
        broad = j // 4
        stacked = jnp.concatenate(parts, axis=0).astype(BF)
        low, high = stacked[:, 0:128].T, stacked[:, 128:256].T
        even = par == 0
        at[8 * broad + 4 * par + j - 4 * broad] = jnp.where(even, low, high)
        sbuf[j] = jnp.where(even, high, low)
        out_desc(j).start()

    def factor_of(h):
        return jnp.where(h < 8, NARROW_SCALE, BROAD_SCALE).astype(F32)

    def attention(block0, count, last, hook):
        def rows_of(b):
            return slice((block0 + b) * 256, (block0 + b) * 256 + 256)

        def here_of(b):
            return slice(b * 256, b * 256 + 256)

        def score(h, slot, b):
            broad = h // 8
            block = (1 - broad) * (h // 2) + broad * (h - 4)
            lanes = pl.ds(pl.multiple_of(block * 128, 128), 128)
            keys = jnp.concatenate([kp[rows_of(b), lanes], kr[rows_of(b), :]], axis=1)
            scores = jnp.dot(keys, qmt[h], preferred_element_type=F32)
            s_buf[slot, here_of(b), :] = scores
            return jnp.max(scores.reshape(32, 8, 256), axis=0)

        def settle(h, peak):
            top = jnp.max(peak, axis=0, keepdims=True)
            if last:
                top = jnp.maximum(top, top_buf[0, h])
            top_buf[int(last), h] = top
            return top

        def soften(slot, b, top, factor):
            p_buf[slot, here_of(b), :] = jnp.exp2(
                (s_buf[slot, here_of(b), :] - top) * factor
            ).astype(BF)

        def gather(h, slot):
            keys = slice(block0 * 256, (block0 + count) * 256)
            return jnp.dot(
                vt[h, :, keys], p_buf[slot, : count * 256, :], preferred_element_type=F32
            )

        def all_scores(h, slot):
            peak = score(h, slot, 0)
            for b in range(1, count):
                peak = jnp.maximum(peak, score(h, slot, b))
            return settle(h, peak)

        first_top = all_scores(0, 0)
        for b in range(count):
            soften(0, b, first_top, factor_of(0))
        second_top = all_scores(1, 1)

        def step(i, top):
            hook(i)
            parts = []
            for k in range(2):
                h = 2 * i + k
                ahead = jnp.minimum(h + 2, 15)
                factor = factor_of(jnp.minimum(h + 1, 15))
                sums = gather(h, k)
                peak = None
                for b in range(count):
                    found = score(ahead, k, b)
                    peak = found if peak is None else jnp.maximum(peak, found)
                    soften(1 - k, b, top, factor)
                if last:
                    kept = jnp.exp2((top_buf[0, h] - top_buf[1, h]) * factor_of(h))
                    whole = acc_buf[h] * kept + sums
                    parts.append(whole[0:64] / whole[64:65])
                else:
                    acc_buf[h] = sums
                top = settle(ahead, peak)
            if last:
                finish_pair(i, parts)
            return top

        lax.fori_loop(0, 8, step, second_top)

    for step in range(Z_EARLY + 1, 6):
        z_step(step)
    project_steps(1, 5)
    z_step(6)

    def hook(i):
        @pl.when(i == HOOK)
        def _():
            z_step(7)

    attention(0, 5, False, hook)
    z_step(8)
    project_steps(6, 8)
    attention(5, 3, True, lambda i: None)

    def landed(j, carry):
        broad = j // 4
        src = 8 * broad + 4 * (1 - par) + j - 4 * broad
        pltpu.make_async_remote_copy(
            at.at[src], at.at[src], o_send.at[j], o_recv.at[j],
            device_id={"sp": mate}, device_id_type=MESH,
        ).wait_recv()
        out_desc(j).wait_send()
        return carry

    lax.fori_loop(0, 8, landed, 0)
    for which, out in enumerate((out_n, out_b)):
        values = [at[8 * which + i].astype(F32) for i in range(8)]
        squares = sum(v * v for v in values)
        mean = jnp.sum(squares, axis=-1, keepdims=True) * (1.0 / 1024)
        scale = lax.rsqrt(mean + EPSILON)
        for i in range(8):
            out[0, :, 128 * i : 128 * i + 128] = (values[i] * scale).astype(BF)

    for make in started:
        make().wait_send()


def on_device(ql, kl, rk, qg, kg, nq, bq, nk, nv, bk, bv):
    vmem = pl.BlockSpec(memory_space=pltpu.VMEM)
    hbm = pl.BlockSpec(memory_space=pl.ANY)
    dma = pltpu.SemaphoreType.DMA
    return pl.pallas_call(
        body,
        out_shape=[jax.ShapeDtypeStruct((1, 128, 1024), BF)] * 2,
        in_specs=[hbm] * 15,
        out_specs=[vmem] * 2,
        scratch_shapes=[
            pltpu.VMEM((24, 768), BF),
            pltpu.VMEM((24, 1280), BF),
            pltpu.VMEM((96, 8, 2048), BF),
            pltpu.VMEM((512, 2560), BF),
            pltpu.VMEM((16, 128, 512), BF),
            pltpu.VMEM((16, 32, 128), BF),
            pltpu.VMEM((2, 128, 768), BF),
            pltpu.VMEM((768, 2048), BF),
            pltpu.VMEM((1024, 512), BF),
            pltpu.VMEM((16, 256, 256), BF),
            pltpu.VMEM((2048, 1536), BF),
            pltpu.VMEM((2048, 128), BF),
            pltpu.VMEM((16, 80, 2048), BF),
            pltpu.VMEM((16, 128, 128), BF),
            pltpu.VMEM((8, 128, 128), BF),
            pltpu.VMEM((256, 128), F32),
            pltpu.VMEM((256, 128), F32),
            pltpu.VMEM((2, 1280, 256), F32),
            pltpu.VMEM((2, 1280, 256), BF),
            pltpu.VMEM((16, 80, 256), F32),
            pltpu.VMEM((2, 16, 1, 256), F32),
            pltpu.VMEM((1, 128, 768), BF),
            pltpu.VMEM((1, 128, 512), BF),
            pltpu.VMEM((1, 32, 128), BF),
            pltpu.VMEM((768,), F32),
            pltpu.VMEM((512,), F32),
            pltpu.VMEM((8, 128), F32),
            pltpu.VMEM((8, 128), F32),
            pltpu.VMEM((256, 128), F32),
            pltpu.VMEM((256, 128), F32),
            dma((15,)),
            dma((16,)),
            dma((16,)),
            dma((64,)),
            dma((64,)),
            dma((64,)),
            dma((64,)),
            dma((2, 8 * (PZ + 1))),
            dma((2, 8 * (PZ + 1))),
            dma((1,)),
            dma((1,)),
            dma((8,)),
            dma((8,)),
        ],
        compiler_params=pltpu.CompilerParams(
            collective_id=0, has_side_effects=True, vmem_limit_bytes=VMEM_LIMIT
        ),
        name="latent_attention",
    )(
        ql, kl, jnp.swapaxes(rk, 1, 2), qg, kg,
        *(jnp.asarray(t) for t in rotary_tables()),
        nq, bq, nk, nv, bk, bv,
    )


def solution(mesh):
    in_specs = (
        P("dp", "sp", None),
        P("dp", "sp", None),
        P("dp", "sp", None),
        P(),
        P(),
        P("dp", None),
        P("dp", None),
        P("dp", None),
        P("dp", None),
        P("dp", None),
        P("dp", None),
    )
    out_specs = (P("dp", "sp", None), P("dp", "sp", None))
    return jax.shard_map(
        on_device, mesh=mesh, in_specs=in_specs, out_specs=out_specs, check_vma=False
    )
```

```python
import functools
import math

import jax
import jax.numpy as jnp
import numpy as np
from jax import lax
from jax.experimental import pallas as pl
from jax.experimental.pallas import tpu as pltpu
from jax.sharding import PartitionSpec as P

EPSILON = 1e-06
ROTARY_BASE = 10000.0
PZ = 4
Z_EARLY = 4
HOOK = 4
VMEM_LIMIT = 60 * 1024 * 1024
BF = jnp.bfloat16
F32 = jnp.float32
MESH = pl.DeviceIdType.MESH
NARROW_SCALE = 96 ** -0.5 * math.log2(math.e)
BROAD_SCALE = 160 ** -0.5 * math.log2(math.e)


def rotary_tables():
    frequency = ROTARY_BASE ** (-np.arange(16, dtype=np.float64) / 16)
    lanes = np.tile(frequency, 8)
    coarse = (256.0 * np.arange(8))[:, None] * lanes[None, :]
    fine = np.arange(256.0)[:, None] * lanes[None, :]
    return tuple(
        np.asarray(t, np.float32)
        for t in (np.cos(coarse), np.sin(coarse), np.cos(fine), np.sin(fine))
    )


def lane_iota(shape):
    return lax.broadcasted_iota(jnp.int32, shape, len(shape) - 1)


def row_iota(shape):
    return lax.broadcasted_iota(jnp.int32, shape, 0)


def normalize(latent, gain_row):
    values = latent.astype(F32)
    scaled = values * lax.rsqrt(jnp.mean(values * values, axis=-1, keepdims=True) + EPSILON)
    return (scaled * gain_row[None, :]).astype(BF)


def rotate(values, cosine, signed_sine):
    first = lane_iota(values.shape) % 32 < 16
    swapped = jnp.where(first, pltpu.roll(values, 112, 1), pltpu.roll(values, 16, 1))
    return values * cosine + swapped * signed_sine


def take(columns, segments):
    rows = columns.shape[0]
    lane = lane_iota((rows, 128))
    out, dest = None, 0
    for start, width in segments:
        tile, off = start // 128, start % 128
        span = 128 if off + width <= 128 else 256
        window = columns[:, tile * 128 : tile * 128 + span]
        shift = (dest - off) % span
        moved = pltpu.roll(window, shift, 1)[:, :128] if shift else window[:, :128]
        out = moved if out is None else jnp.where(lane >= dest, moved, out)
        dest += width
    return out


def body(
    ql, kl, rk, qg, kg, ca, sa, cb, sb, nq, bq, nk, nv, bk, bv,
    out_n, out_b,
    raw_n, raw_b, wq8, wkv, kv, rt, qn, wq, wvt, qmt, kp, kr, vt, at, sbuf, cos_t, sin_t,
    s_buf, p_buf, acc_buf, top_buf,
    v_ql, v_kl, v_rk, v_qg, v_kg, v_ca, v_sa, v_cb, v_sb,
    in_sem, f_send, f_recv, g_send, g_recv, dd_send, dd_recv, z_send, z_recv,
    q_send, q_recv, o_send, o_recv,
):
    z = lax.axis_index("sp")
    d = lax.axis_index("dp")
    par = lax.rem(z, 2)
    core = lax.rem(d, 2)
    chip = d // 2
    here = (lax.rem(chip, 4), chip // 4)
    partner_core = d + 1 - 2 * core
    mate = z + 1 - 2 * par
    zs = {k: lax.rem(z + k + 16, 16) for k in range(-8, 9)}

    where = {}
    for t in range(2):
        along = [[lax.rem(here[axis] + k, 4) for k in range(4)] for axis in (t, 1 - t)]
        for a in range(4):
            for b in range(4):
                xy = (along[0][a], along[1][b]) if t == 0 else (along[1][b], along[0][a])
                where[t, a, b] = (xy[1] * 4 + xy[0]) * 2 + core

    def cols(ref, width):
        return ref.at[:, pl.ds(pl.multiple_of(par * width, 128), width)]

    barrier = pltpu.get_barrier_semaphore()
    near = [{"sp": zs[1]}, {"sp": zs[-1]}, {"dp": partner_core}]
    near += [{"dp": where[t, k, 0]} for t in range(2) for k in (1, 3)]
    for who in near:
        pl.semaphore_signal(barrier, inc=1, device_id=who, device_id_type=MESH)

    own_rows = pl.ds(pl.multiple_of(d * 16, 16), 16)
    pairs = [
        (cols(nk, 512), wkv.at[own_rows, pl.ds(0, 512)]),
        (cols(bk, 1024), wkv.at[own_rows, pl.ds(512, 1024)]),
        (cols(nv, 512), wkv.at[own_rows, pl.ds(1536, 512)]),
        (cols(bv, 512), wkv.at[own_rows, pl.ds(2048, 512)]),
        (cols(nq, 768), raw_n),
        (cols(bq, 1280), raw_b),
        (kl, v_kl), (kg, v_kg), (rk, v_rk), (ca, v_ca), (sa, v_sa), (cb, v_cb), (sb, v_sb),
        (ql, v_ql), (qg, v_qg),
    ]
    loads = [
        pltpu.make_async_copy(src, dst, in_sem.at[i]) for i, (src, dst) in enumerate(pairs)
    ]
    for load in loads:
        load.start()

    def arrange_columns():
        wn, wb = raw_n[...].astype(F32), raw_b[...].astype(F32)
        blocks = [take(wn, [(192 * j, 64), (192 * j + 96, 64)]) for j in range(4)]
        blocks += [take(wb, [(160 * h, 128)]) for h in range(8)]
        for w, size in ((wn, 96), (wb, 160)):
            for g in range(0, 8, 4):
                pieces = [(size * h + size - 32, 32) for h in range(g, g + 4)]
                blocks.append(take(w, pieces))
        for i, block in enumerate(blocks):
            for t in range(3):
                wq8[3 * d + t, :, 128 * i : 128 * i + 128] = block[8 * t : 8 * t + 8].astype(BF)

    def own_pair():
        kv[z] = normalize(v_kl[0], v_kg[...])
        half = pl.ds(pl.multiple_of(par * 128, 128), 128)
        coarse = pl.ds(z // 2, 1)
        cosine = v_ca[coarse, :] * v_cb[...] - v_sa[coarse, :] * v_sb[...]
        sine = v_sa[coarse, :] * v_cb[...] + v_ca[coarse, :] * v_sb[...]
        cos_t[...] = cosine
        sin_t[...] = jnp.where(lane_iota(sine.shape) % 32 < 16, -sine, sine)
        own_rope = v_rk[0].astype(F32)
        rope4 = jnp.concatenate([own_rope] * 4, axis=0).T
        rope4 = rotate(rope4, cos_t[half, :], sin_t[half, :])
        rt[z] = rope4.T[:32].astype(BF)

    started = []

    def start(make):
        make().start()
        started.append(make)

    def piece(t, slot, h):
        if t == 0:
            return wq8.at[pl.ds(3 * slot, 3), :, pl.ds(h * 1024, 1024)]
        return wkv.at[pl.ds(pl.multiple_of(16 * slot, 16), 16), pl.ds(h * 1280, 1280)]

    def xy_desc(t, a, b, h, send, recv, to):
        ref = piece(t, where[t, a, b], h)
        return pltpu.make_async_remote_copy(
            ref, ref, send, recv, device_id={"dp": to}, device_id_type=MESH
        )

    def f_send_copy(t, a, h, to):
        named = (a - to) % 4
        index = (t * 4 + named) * 2 + h
        return lambda: xy_desc(
            t, a, 0, h, f_send.at[index], f_recv.at[index], where[t, to % 4, 0]
        )

    def g_send_copy(t, a, b, h, to):
        named = (b - to) % 4
        index = ((t * 4 + a) * 4 + named) * 2 + h
        return lambda: xy_desc(
            t, a, b, h, g_send.at[index], g_recv.at[index], where[t, 0, to % 4]
        )

    def d_copy(t, a, b, h):
        index = ((t * 4 + a) * 4 + b) * 2 + h
        return lambda: xy_desc(
            t, a, b, h, dd_send.at[index], dd_recv.at[index], partner_core
        )

    def column(t, a, h):
        for to in (1, -1):
            start(g_send_copy(t, a, 0, h, to))
        start(d_copy(t, a, 0, h))

    def f_event(t, a, h):
        index = (t * 4 + a) * 2 + h
        xy_desc(t, a, 0, h, f_send.at[index], f_recv.at[index], d).wait_recv()
        if (a, h) == (3, 0):
            start(f_send_copy(t, a, h, 1))
        if (a, h) == (1, 1):
            start(f_send_copy(t, a, h, -1))
        column(t, a, h)

    def g_event(t, a, b, h):
        index = ((t * 4 + a) * 4 + b) * 2 + h
        xy_desc(t, a, b, h, g_send.at[index], g_recv.at[index], d).wait_recv()
        if (b, h) == (3, 0):
            start(g_send_copy(t, a, b, h, 1))
        if (b, h) == (1, 1):
            start(g_send_copy(t, a, b, h, -1))
        start(d_copy(t, a, b, h))

    rows_z = 128 // PZ

    def z_desc(way, step, i, slot):
        ref = rt.at[slot] if i == PZ else kv.at[slot, pl.ds(i * rows_z, rows_z)]
        index = (step - 1) * (PZ + 1) + i
        return pltpu.make_async_remote_copy(
            ref, ref, z_send.at[way, index], z_recv.at[way, index],
            device_id={"sp": zs[1 - 2 * way]}, device_id_type=MESH,
        )

    def z_copy(way, step, i):
        return lambda: z_desc(way, step, i, zs[-(1 - 2 * way) * (step - 1)])

    def z_pieces(way, step):
        if step < 8:
            return [PZ] + list(range(PZ))
        return [PZ] + list(range(PZ // 2)) if way == 0 else list(range(PZ // 2, PZ))

    def z_event(step, i):
        for way in range(2):
            if i not in z_pieces(way, step):
                continue
            z_desc(way, step, i, zs[-(1 - 2 * way) * step]).wait_recv()
            if step < 8 and i in z_pieces(way, step + 1):
                start(z_copy(way, step + 1, i))

    def z_step(step):
        for i in z_pieces(0, 1):
            z_event(step, i)

    def send_weights(t):
        for h in range(2):
            for to in (1, -1):
                start(f_send_copy(t, 0, h, to))
        for h in range(2):
            column(t, 0, h)

    for load in loads[:4]:
        load.wait()
    pl.semaphore_wait(barrier, 7)
    send_weights(1)
    for load in loads[4:6]:
        load.wait()
    arrange_columns()
    for load in loads[6:13]:
        load.wait()
    own_pair()
    send_weights(0)
    for load in loads[13:]:
        load.wait()
    qn[par] = normalize(v_ql[0], v_qg[...])
    for i in z_pieces(0, 1):
        for way in range(2):
            start(z_copy(way, 1, i))
    for h in range(16):
        vt[h, 64:80, :] = jnp.ones((16, 2048), BF)
    mine = qn.at[par]
    start(
        lambda: pltpu.make_async_remote_copy(
            mine, mine, q_send.at[0], q_recv.at[0], device_id={"sp": mate}, device_id_type=MESH
        )
    )

    events = []
    for t in (1, 0):
        for h in range(2):
            for a in (1, 3):
                events.append((3.0 + h, f_event, (t, a, h)))
            events.append((6.0 + h, f_event, (t, 2, h)))
            for b in (1, 3):
                events.append((5.0 + h, g_event, (t, 0, b, h)))
                events.append((8.0 + h, g_event, (t, 1, b, h)))
                events.append((10.0 + h, g_event, (t, 3, b, h)))
                events.append((13.0 + h, g_event, (t, 2, b, h)))
            events.append((8.5 + h, g_event, (t, 0, 2, h)))
            events.append((11.5 + h, g_event, (t, 1, 2, h)))
            events.append((13.5 + h, g_event, (t, 3, 2, h)))
            events.append((16.5 + h, g_event, (t, 2, 2, h)))
    for step in range(1, Z_EARLY + 1):
        for k, i in enumerate(z_pieces(0, 1)):
            events.append((3.7 * step - 2 + 0.5 * k, z_event, (step, i)))
    for _, event, what in sorted(events, key=lambda e: e[0]):
        event(*what)
    for t in (1, 0):
        for a in range(4):
            for b in range(4):
                for h in range(2):
                    index = ((t * 4 + a) * 4 + b) * 2 + h
                    ref = piece(t, where[t, a, b] + 1 - 2 * core, h)
                    pltpu.make_async_remote_copy(
                        ref, ref, dd_send.at[index], dd_recv.at[index],
                        device_id={"dp": partner_core}, device_id_type=MESH,
                    ).wait_recv()
        if t == 1:
            for i in range(8):
                wvt[128 * i : 128 * i + 128, :] = wkv[:, 1536 + 128 * i : 1664 + 128 * i].T
    theirs = qn.at[1 - par]
    pltpu.make_async_remote_copy(
        theirs, theirs, q_send.at[0], q_recv.at[0], device_id={"sp": mate}, device_id_type=MESH
    ).wait_recv()

    def pack_rows(g, carry):
        pair = jnp.concatenate([wq8[2 * g].astype(F32), wq8[2 * g + 1].astype(F32)], axis=0)
        wq[pl.ds(pl.multiple_of(16 * g, 16), 16), :] = pair.astype(BF)
        return carry

    lax.fori_loop(0, 48, pack_rows, 0)

    tokens = jnp.concatenate([qn[0], qn[1]], axis=0)
    group = row_iota((128, 256)) // 32
    side = row_iota((128, 256)) // 64
    nothing = jnp.zeros((128, 256), BF)
    for pair in range(8):
        both = jnp.dot(tokens, wq[:, 256 * pair : 256 * pair + 256], preferred_element_type=F32)
        for k in range(2):
            block = 2 * pair + k
            part = both[:, 128 * k : 128 * k + 128]
            if block >= 12:
                part = rotate(part, cos_t[...], sin_t[...])
            turned = part.astype(BF).T
            if block < 4:
                for s in range(2):
                    qmt[2 * block + s, 0:128, :] = jnp.where(side == s, turned, nothing)
            elif block < 12:
                qmt[block + 4, 0:128, :] = turned
            else:
                for g in range(4):
                    head = 4 * (block - 12) + g
                    qmt[head, 128:256, :] = jnp.where(group == g, turned, nothing)

    def project(b, one, two):
        rows = pl.ds(pl.multiple_of(256 * b, 256), 256)
        x = jnp.concatenate([kv[one], kv[two]], axis=0)
        for i in range(6):
            kp[rows, 256 * i : 256 * i + 256] = jnp.dot(
                x, wkv[:, 256 * i : 256 * i + 256], preferred_element_type=F32
            ).astype(BF)
        for i in range(4):
            turned = lax.dot_general(
                wvt[256 * i : 256 * i + 256, :], x, (((1,), (1,)), ((), ())),
                preferred_element_type=F32,
            ).astype(BF)
            for k in range(4):
                vt[4 * i + k, 0:64, rows] = turned[64 * k : 64 * k + 64]
        for k, slot in enumerate((one, two)):
            own = rt[slot].astype(F32)
            kr[pl.ds(pl.multiple_of(256 * b + 128 * k, 128), 128), :] = (
                jnp.concatenate([own, own, own, own], axis=0).T.astype(BF)
            )

    def project_steps(first, last):
        def one_step(s, carry):
            project(s - 1, lax.rem(z + 16 - s, 16), lax.rem(z + lax.rem(s, 8) + 16, 16))
            return carry

        lax.fori_loop(first, last + 1, one_step, 0)

    def out_desc(j):
        broad = j // 4
        dst = 8 * broad + 4 * par + j - 4 * broad
        return pltpu.make_async_remote_copy(
            sbuf.at[j], at.at[dst], o_send.at[j], o_recv.at[j],
            device_id={"sp": mate}, device_id_type=MESH,
        )

    def finish_pair(j, parts):
        broad = j // 4
        stacked = jnp.concatenate(parts, axis=0).astype(BF)
        low, high = stacked[:, 0:128].T, stacked[:, 128:256].T
        even = par == 0
        at[8 * broad + 4 * par + j - 4 * broad] = jnp.where(even, low, high)
        sbuf[j] = jnp.where(even, high, low)
        out_desc(j).start()

    def factor_of(h):
        return jnp.where(h < 8, NARROW_SCALE, BROAD_SCALE).astype(F32)

    def attention(block0, count, last, hook):
        def rows_of(b):
            return slice((block0 + b) * 256, (block0 + b) * 256 + 256)

        def here_of(b):
            return slice(b * 256, b * 256 + 256)

        def score(h, slot, b):
            broad = h // 8
            block = (1 - broad) * (h // 2) + broad * (h - 4)
            lanes = pl.ds(pl.multiple_of(block * 128, 128), 128)
            keys = jnp.concatenate([kp[rows_of(b), lanes], kr[rows_of(b), :]], axis=1)
            scores = jnp.dot(keys, qmt[h], preferred_element_type=F32)
            s_buf[slot, here_of(b), :] = scores
            return jnp.max(scores.reshape(32, 8, 256), axis=0)

        def settle(h, peak):
            top = jnp.max(peak, axis=0, keepdims=True)
            if last:
                top = jnp.maximum(top, top_buf[0, h])
            top_buf[int(last), h] = top
            return top

        def soften(slot, b, top, factor):
            p_buf[slot, here_of(b), :] = jnp.exp2(
                (s_buf[slot, here_of(b), :] - top) * factor
            ).astype(BF)

        def gather(h, slot):
            keys = slice(block0 * 256, (block0 + count) * 256)
            return jnp.dot(
                vt[h, :, keys], p_buf[slot, : count * 256, :], preferred_element_type=F32
            )

        def all_scores(h, slot):
            peak = score(h, slot, 0)
            for b in range(1, count):
                peak = jnp.maximum(peak, score(h, slot, b))
            return settle(h, peak)

        first_top = all_scores(0, 0)
        for b in range(count):
            soften(0, b, first_top, factor_of(0))
        second_top = all_scores(1, 1)

        def step(i, top, tail=False):
            if not tail:
                hook(i)
            parts = []
            for k in range(2):
                h = 2 * i + k
                ahead = jnp.minimum(h + 2, 15)
                factor = factor_of(jnp.minimum(h + 1, 15))
                sums = gather(h, k)
                peak = None
                for b in range(count):
                    if not tail:
                        found = score(ahead, k, b)
                        peak = found if peak is None else jnp.maximum(peak, found)
                    if not tail or k == 0:
                        soften(1 - k, b, top, factor)
                if last:
                    kept = jnp.exp2((top_buf[0, h] - top_buf[1, h]) * factor_of(h))
                    whole = acc_buf[h] * kept + sums
                    parts.append(whole[0:64] / whole[64:65])
                else:
                    acc_buf[h] = sums
                if not tail:
                    top = settle(ahead, peak)
            if last:
                finish_pair(i, parts)
            return top

        step(7, lax.fori_loop(0, 7, step, second_top), tail=True)

    for step in range(Z_EARLY + 1, 6):
        z_step(step)
    project_steps(1, 5)
    z_step(6)

    def hook(i):
        @pl.when(i == HOOK)
        def _():
            z_step(7)

    attention(0, 5, False, hook)
    z_step(8)
    project_steps(6, 8)
    attention(5, 3, True, lambda i: None)

    def landed(j, carry):
        broad = j // 4
        src = 8 * broad + 4 * (1 - par) + j - 4 * broad
        pltpu.make_async_remote_copy(
            at.at[src], at.at[src], o_send.at[j], o_recv.at[j],
            device_id={"sp": mate}, device_id_type=MESH,
        ).wait_recv()
        out_desc(j).wait_send()
        return carry

    lax.fori_loop(0, 8, landed, 0)
    for which, out in enumerate((out_n, out_b)):
        values = [at[8 * which + i].astype(F32) for i in range(8)]
        squares = sum(v * v for v in values)
        mean = jnp.sum(squares, axis=-1, keepdims=True) * (1.0 / 1024)
        scale = lax.rsqrt(mean + EPSILON)
        for i in range(8):
            out[0, :, 128 * i : 128 * i + 128] = (values[i] * scale).astype(BF)

    for make in started:
        make().wait_send()


def on_device(ql, kl, rk, qg, kg, nq, bq, nk, nv, bk, bv):
    vmem = pl.BlockSpec(memory_space=pltpu.VMEM)
    hbm = pl.BlockSpec(memory_space=pl.ANY)
    dma = pltpu.SemaphoreType.DMA
    return pl.pallas_call(
        body,
        out_shape=[jax.ShapeDtypeStruct((1, 128, 1024), BF)] * 2,
        in_specs=[hbm] * 15,
        out_specs=[vmem] * 2,
        scratch_shapes=[
            pltpu.VMEM((24, 768), BF),
            pltpu.VMEM((24, 1280), BF),
            pltpu.VMEM((96, 8, 2048), BF),
            pltpu.VMEM((512, 2560), BF),
            pltpu.VMEM((16, 128, 512), BF),
            pltpu.VMEM((16, 32, 128), BF),
            pltpu.VMEM((2, 128, 768), BF),
            pltpu.VMEM((768, 2048), BF),
            pltpu.VMEM((1024, 512), BF),
            pltpu.VMEM((16, 256, 256), BF),
            pltpu.VMEM((2048, 1536), BF),
            pltpu.VMEM((2048, 128), BF),
            pltpu.VMEM((16, 80, 2048), BF),
            pltpu.VMEM((16, 128, 128), BF),
            pltpu.VMEM((8, 128, 128), BF),
            pltpu.VMEM((256, 128), F32),
            pltpu.VMEM((256, 128), F32),
            pltpu.VMEM((2, 1280, 256), F32),
            pltpu.VMEM((2, 1280, 256), BF),
            pltpu.VMEM((16, 80, 256), F32),
            pltpu.VMEM((2, 16, 1, 256), F32),
            pltpu.VMEM((1, 128, 768), BF),
            pltpu.VMEM((1, 128, 512), BF),
            pltpu.VMEM((1, 32, 128), BF),
            pltpu.VMEM((768,), F32),
            pltpu.VMEM((512,), F32),
            pltpu.VMEM((8, 128), F32),
            pltpu.VMEM((8, 128), F32),
            pltpu.VMEM((256, 128), F32),
            pltpu.VMEM((256, 128), F32),
            dma((15,)),
            dma((16,)),
            dma((16,)),
            dma((64,)),
            dma((64,)),
            dma((64,)),
            dma((64,)),
            dma((2, 8 * (PZ + 1))),
            dma((2, 8 * (PZ + 1))),
            dma((1,)),
            dma((1,)),
            dma((8,)),
            dma((8,)),
        ],
        compiler_params=pltpu.CompilerParams(
            collective_id=0, has_side_effects=True, vmem_limit_bytes=VMEM_LIMIT
        ),
        name="latent_attention",
    )(
        ql, kl, jnp.swapaxes(rk, 1, 2), qg, kg,
        *(jnp.asarray(t) for t in rotary_tables()),
        nq, bq, nk, nv, bk, bv,
    )


def solution(mesh):
    in_specs = (
        P("dp", "sp", None),
        P("dp", "sp", None),
        P("dp", "sp", None),
        P(),
        P(),
        P("dp", None),
        P("dp", None),
        P("dp", None),
        P("dp", None),
        P("dp", None),
        P("dp", None),
    )
    out_specs = (P("dp", "sp", None), P("dp", "sp", None))
    return jax.shard_map(
        on_device, mesh=mesh, in_specs=in_specs, out_specs=out_specs, check_vma=False
    )
```
